32 devices in a mesh: sp: 8 (over z, core), tp: 4 (over y, x).
Axes of the slice: x: 2, y: 2, z: 4, core: 2. Of those that a mesh axis runs over, the one named last changes fastest.
Arguments:
- resid: bfloat16 [1536, 2048], P('sp', 'tp'), may hold values from -12 to 12
- conv_value: bfloat16 [1536, 2048], P('sp', 'tp'), may hold values from -80 to 80
- conv_gate: bfloat16 [1536, 2048], P('sp', 'tp'), may hold values from -6 to 6
- depth_kernel: float32 [31, 2048], P(None, 'tp'), may hold values from -1 to 1
- chan_gain: float32 [2048], P('tp'), may hold values from 0.1 to 1.9
- point_weight: bfloat16 [2048, 2048], P('tp'), may hold values from -0.125 to 0.125
- mix_gain: float32 [2048], replicated, may hold values from 0.1 to 1.9
- out_weight: bfloat16 [2048, 2048], P(None, 'tp'), may hold values from -0.125 to 0.125
- norm_gain: float32 [2048], P('tp'), may hold values from 0.1 to 1.9
- route_ids: int32 [1536, 4], P('sp'), may hold values from 0 to 31, all different within a row; in each aligned block of 192 rows (0 to 191, 192 to 383, ...) at most 32 rows name the same one
- route_weights: float32 [1536, 4], P('sp'), may hold values from 0.05 to 0.5
- gate_experts: bfloat16 [32, 2048, 4096], P('sp', None, 'tp'), may hold values from -0.3125 to 0.3125
- up_experts: bfloat16 [32, 2048, 4096], P('sp', None, 'tp'), may hold values from -0.3125 to 0.3125
- down_experts: bfloat16 [32, 4096, 2048], P('sp', 'tp'), may hold values from -0.09375 to 0.09375
Outputs:
- result: bfloat16 [1536, 2048], P('sp', 'tp')
The draws below stay inside these ranges and needn't reach their ends.
Inputs may be any that keep to these rules, and one draw needn't show every extreme that they name: `route_ids`: each row names 4 different experts; among the 192 rows of one index of sp no expert is named by more than 32 rows, and in some such block an expert is named by exactly 32.
All inputs are finite; a program needn't handle non-finite values.
Results may differ from the reference program's by a relative error of at most 0.024.
Values may be sent and summed in bfloat16 or wider, within the bound.
A program may use at most 128 MiB of HBM per device.

```python
import math
import jax
import jax.numpy as jnp
import numpy as np
from jax import lax

D = 2048
CONV_CH = 2048
F = 4096
E = 32
TOPK = 4
WIDTH = 31
TOK_DEV = 192
TOKENS = 1536
CAP = 32
N_SP = 8
N_TP = 4


def scaled_draw(key, rows, columns, top):
    first, second = jax.random.split(key, 2)
    column_scale = top ** (jnp.arange(columns, dtype=jnp.float32) / columns)
    row_scale = jnp.exp(jax.random.uniform(second, (rows, 1), jnp.float32, -0.69, 0.69))
    base = jax.random.truncated_normal(first, -4.0, 4.0, (rows, columns), jnp.float32)
    return base * column_scale * row_scale


def draw_resid(key, part):
    values = scaled_draw(jax.random.fold_in(key, 11), TOKENS, D, 3.0) * 0.5
    return values.astype(jnp.bfloat16)


def draw_conv_value(key, part):
    values = scaled_draw(jax.random.fold_in(key, 23), TOKENS, CONV_CH, 10.0)
    return values.astype(jnp.bfloat16)


def levels(stream_key, dims, shards, least, high):
    level, own = 1.0, jax.random.fold_in(stream_key, 6)
    for dim, shards_of in shards:
        heights = jnp.exp(jax.random.uniform(jax.random.fold_in(own, dim), (shards_of,), jnp.float32, least / len(shards), high / len(shards)))
        level = level * jnp.repeat(heights, dims[dim] // shards_of).reshape([-1 if axis == dim else 1 for axis in range(len(dims))])
    return level


def assign_block(stream_key, own, number, rows, amount, top, reach, skew):
    order = jax.random.permutation(stream_key, amount)
    crowded, usual = load_shares(amount, rows * top, reach, skew, True), load_shares(amount, rows * top, reach, skew, False)
    places = jnp.arange(amount)

    def named(lengths, turn):
        used = int((lengths > 0).sum())
        fixed = max(1, used // 4)
        shifted = fixed + (places - fixed + turn * (used - fixed)) % max(1, amount - fixed)
        return jnp.zeros((amount,), jnp.int32).at[order[jnp.where(places < fixed, places, shifted)]].set(jnp.asarray(lengths, jnp.int32))

    lengths = jnp.where(number % 4 == 0, named(crowded, number // 4), named(usual, number - number // 4 - 1))
    mixed = jax.random.permutation(jax.random.fold_in(own, 3), amount)
    source_of, receiver = mixed[0:amount // 2 * 2:2], mixed[1:amount // 2 * 2:2]
    margin = jnp.minimum(lengths[source_of] - 1, reach - lengths[receiver]) // 2
    margin = jnp.where((source_of == order[0]) | (receiver == order[0]) | (lengths[receiver] == 0), 0, jnp.maximum(margin, 0))
    shifted = jax.random.randint(jax.random.fold_in(own, 4), (amount // 2,), 0, 1 << 20) % (margin + 1)
    lengths = lengths.at[source_of].add(-shifted).at[receiver].add(shifted)
    members = jnp.searchsorted(jnp.cumsum(lengths), jnp.arange(rows * top), side="right").astype(jnp.int32)
    grid = members.reshape(top, rows).T
    grid = grid[jax.random.permutation(jax.random.fold_in(own, 1), rows)]
    turn = jax.random.randint(jax.random.fold_in(own, 2), (rows, 1), 0, top)
    return jnp.take_along_axis(grid, (jnp.arange(top)[None, :] + turn) % top, axis=1)


def load_shares(amount, total, bound, slope, full):
    weights = [(1 << 20) // math.isqrt(standing ** slope) + 1 for standing in range(1, amount + 1)]
    largest = bound if full else min(bound, max(-(-total // amount), total * weights[0] // sum(weights)))
    least = 1 if total - largest >= amount - 1 else 0
    holding, spare = [largest] + [least] * (amount - 1), total - largest - least * (amount - 1)
    while spare > 0:
        movable = [i for i in range(1, amount) if holding[i] < largest] or [i for i in range(1, amount) if holding[i] < bound]
        pool, left = sum([weights[i] for i in movable]), spare
        for i in movable:
            addition = min(bound - holding[i], max(1, left * weights[i] // pool), spare)
            holding[i] = holding[i] + addition
            spare = spare - addition
    return np.array(holding)


def gaussian(key, extent, scale, most, pieces=(), kind=jnp.bfloat16):
    array = jax.random.normal(key, extent, jnp.float32) * scale
    if len(pieces) > 0:
        array = levels(key, extent, pieces, -0.22, 0.18) * array
    return jnp.clip(array, min=-most, max=most).astype(kind)


def setup_inputs(seed: int = 0) -> dict:
    key_of = jax.random.split(jax.random.key(seed), 15)
    resid = draw_resid(jax.random.fold_in(key_of[14], 71), 0)
    conv_value = draw_conv_value(jax.random.fold_in(key_of[14], 71), 0)
    conv_gate = gaussian(key_of[2], (TOKENS, CONV_CH), 1.5, 6.0, ((0, 8), (1, 4)))
    depth_kernel = gaussian(key_of[3], (WIDTH, CONV_CH), WIDTH ** -0.5, 1.0, ((1, 4),), jnp.float32)
    chan_gain = jnp.clip(1.0 + 0.18 * jax.random.normal(key_of[4], (CONV_CH,), jnp.float32), 0.1, 1.9)
    point_weight = gaussian(key_of[5], (CONV_CH, CONV_CH), CONV_CH ** -0.5, 0.125, ((0, 4),))
    mix_gain = jnp.clip(1.0 + 0.18 * jax.random.normal(key_of[6], (CONV_CH,), jnp.float32), 0.1, 1.9)
    out_weight = gaussian(key_of[7], (CONV_CH, D), CONV_CH ** -0.5, 0.125, ((1, 4),))
    norm_gain = jnp.clip(1.0 + 0.18 * jax.random.normal(key_of[8], (D,), jnp.float32), 0.1, 1.9)
    route_ids_keys = jax.random.split(jax.random.fold_in(key_of[9], 1), TOKENS // TOK_DEV)
    route_ids_turns = jax.random.permutation(jax.random.fold_in(key_of[9], 3), TOKENS // TOK_DEV)
    route_ids = jax.vmap(lambda own, number: assign_block(jax.random.fold_in(key_of[9], 2), own, number, TOK_DEV, E, TOPK, CAP, 2))(route_ids_keys, route_ids_turns).reshape((TOKENS, TOPK))
    route_weights = jnp.clip(0.05 + 0.45 * jax.random.uniform(key_of[10], (TOKENS, TOPK), jnp.float32) ** levels(key_of[10], (TOKENS, TOPK), ((0, 8),), -0.2, 0.2), 0.05, 0.5)
    gate_experts = gaussian(key_of[11], (E, D, F), (D // 6) ** -0.5, 0.3125, ((0, 8), (2, 4)))
    up_experts = gaussian(key_of[12], (E, D, F), (D // 6) ** -0.5, 0.3125, ((0, 8), (2, 4)))
    down_experts = gaussian(key_of[13], (E, F, D), F ** -0.5, 0.09375, ((0, 8), (1, 4)))
    return dict(resid=resid, conv_value=conv_value, conv_gate=conv_gate, depth_kernel=depth_kernel, chan_gain=chan_gain, point_weight=point_weight, mix_gain=mix_gain, out_weight=out_weight, norm_gain=norm_gain, route_ids=route_ids, route_weights=route_weights, gate_experts=gate_experts, up_experts=up_experts, down_experts=down_experts)


epsilon = 1e-05
clamp_limit = 7.0
swish_slope = 1.702

def rounded_sum(left, right, blocks):
    inner = left.shape[1] // blocks
    total = jnp.zeros((left.shape[0], right.shape[1]), jnp.float32)
    for block in range(blocks):
        part = jnp.dot(left[:, block * inner:(block + 1) * inner], right[block * inner:(block + 1) * inner], preferred_element_type=jnp.float32)
        total = total + lax.optimization_barrier(part.astype(jnp.bfloat16)).astype(jnp.float32)
    return total

def reference(resid, conv_value, conv_gate, depth_kernel, chan_gain, point_weight, mix_gain, out_weight, norm_gain, route_ids, route_weights, gate_experts, up_experts, down_experts):
    gated = (conv_value.astype(jnp.float32) * jax.nn.sigmoid(conv_gate.astype(jnp.float32))).astype(jnp.bfloat16)
    padded = jnp.concatenate([jnp.zeros((WIDTH - 1, CONV_CH), jnp.bfloat16), gated], axis=0)
    conv = jnp.zeros((TOKENS, CONV_CH), jnp.float32)
    for tap in range(WIDTH):
        conv = conv + padded[tap:tap + TOKENS].astype(jnp.float32) * depth_kernel[tap]
    center = conv - lax.optimization_barrier(jnp.mean(conv, axis=1, keepdims=True))
    spread = lax.optimization_barrier(jnp.mean(center * center, axis=1, keepdims=True))
    act = jax.nn.silu(center * lax.rsqrt(spread + epsilon) * chan_gain).astype(jnp.bfloat16)
    point = rounded_sum(act, point_weight, N_TP)
    mixed = (point * lax.rsqrt(lax.optimization_barrier(jnp.mean(point * point, axis=1, keepdims=True)) + epsilon) * mix_gain).astype(jnp.bfloat16)
    middle = (resid.astype(jnp.float32) + jnp.dot(mixed, out_weight, preferred_element_type=jnp.float32)).astype(jnp.bfloat16)
    middle32 = middle.astype(jnp.float32)
    normed = (middle32 * lax.rsqrt(lax.optimization_barrier(jnp.mean(middle32 * middle32, axis=1, keepdims=True)) + epsilon) * norm_gain).astype(jnp.bfloat16)
    flat_ids = route_ids.reshape(-1).astype(jnp.int32)
    flat_weights = route_weights.reshape(-1)
    routed = TOKENS * TOPK
    total = jnp.zeros((TOKENS, D), jnp.float32)
    for expert in range(E):
        found = jnp.nonzero(flat_ids == expert, size=N_SP * CAP, fill_value=routed)[0].astype(jnp.int32)
        valid = found < routed
        token = jnp.minimum(found // TOPK, TOKENS - 1).astype(jnp.int32)
        weight = jnp.where(valid, flat_weights[jnp.minimum(found, routed - 1)], 0.0)
        rows = normed[token]
        gate_pre = jnp.minimum(jnp.dot(rows, gate_experts[expert], preferred_element_type=jnp.float32), clamp_limit)
        up_pre = jnp.clip(jnp.dot(rows, up_experts[expert], preferred_element_type=jnp.float32), -clamp_limit, clamp_limit)
        hidden = (gate_pre * jax.nn.sigmoid(swish_slope * gate_pre) * (up_pre + 1.0)).astype(jnp.bfloat16)
        expert_out = rounded_sum(hidden, down_experts[expert], N_TP).astype(jnp.bfloat16)
        total = total.at[token].add(expert_out.astype(jnp.float32) * weight[:, None])
    return (middle32 + total).astype(jnp.bfloat16)
```

```python
import jax
import jax.numpy as jnp
import functools

from jax import lax
from jax.experimental import pallas as pl
from jax.experimental.pallas import tpu as pltpu
from jax.sharding import PartitionSpec as P

E = 32
TOPK = 4
CAP = 32


epsilon = 1e-05
clamp_limit = 7.0
swish_slope = 1.702


def from_behind(block, axis, distance):
    devices = range(lax.axis_size(axis))
    route = [(i - distance, i) for i in devices if i - distance in devices]
    return lax.ppermute(block, axis, route)


def plain_shards(
    resid,
    conv_value,
    conv_gate,
    depth_kernel,
    chan_gain,
    point_weight,
    mix_gain,
    out_weight,
    norm_gain,
    route_ids,
    route_weights,
    gate_experts,
    up_experts,
    down_experts,
):
    tok_rows, chan_local = conv_value.shape
    feat_local = resid.shape[1]
    lookback = depth_kernel.shape[0] - 1
    gated = (conv_value.astype(jnp.float32) * jax.nn.sigmoid(conv_gate.astype(jnp.float32))).astype(
        jnp.bfloat16
    )
    earlier = from_behind(gated[tok_rows - lookback :], "sp", 1)
    padded = jnp.concatenate([earlier, gated], axis=0)
    conv = jnp.zeros((tok_rows, chan_local), jnp.float32)
    for tap in range(lookback + 1):
        conv = conv + padded[tap : tap + tok_rows].astype(jnp.float32) * depth_kernel[tap]
    chan_total = chan_local * lax.axis_size("tp")
    row_sums, row_squares = lax.psum((jnp.sum(conv, axis=1), jnp.sum(conv * conv, axis=1)), "tp")
    row_mean = row_sums / chan_total
    row_var = row_squares / chan_total - row_mean * row_mean
    act = jax.nn.silu(
        (conv - row_mean[:, None]) * lax.rsqrt(row_var[:, None] + epsilon) * chan_gain
    ).astype(jnp.bfloat16)
    point = lax.psum_scatter(
        jnp.dot(act, point_weight, preferred_element_type=jnp.float32).astype(jnp.bfloat16),
        "tp",
        scatter_dimension=0,
        tiled=True,
    ).astype(jnp.float32)
    mixed = (
        point * lax.rsqrt(jnp.mean(point * point, axis=1, keepdims=True) + epsilon) * mix_gain
    ).astype(jnp.bfloat16)
    branch = jnp.dot(
        lax.all_gather(mixed, "tp", axis=0, tiled=True),
        out_weight,
        preferred_element_type=jnp.float32,
    )
    middle = (resid.astype(jnp.float32) + branch).astype(jnp.bfloat16)
    middle32 = middle.astype(jnp.float32)
    feat_total = feat_local * lax.axis_size("tp")
    squares = lax.psum(jnp.sum(middle32 * middle32, axis=1), "tp")
    normed = (middle32 * lax.rsqrt(squares[:, None] / feat_total + epsilon) * norm_gain).astype(
        jnp.bfloat16
    )
    flat_ids = route_ids.reshape(-1)
    expert_table = (flat_ids[:, None] == jnp.arange(E, dtype=jnp.int32)[None, :]).astype(jnp.int32)
    earlier_count = jnp.cumsum(expert_table, axis=0) - expert_table
    position = jnp.sum(earlier_count * expert_table, axis=1)
    slot_of = flat_ids * CAP + position
    slot_grid = slot_of.reshape(tok_rows, TOPK)
    picker = jnp.any(
        slot_grid[None, :, :] == jnp.arange(E * CAP, dtype=jnp.int32)[:, None, None], axis=2
    ).astype(jnp.bfloat16)
    outgoing = (
        jnp.dot(picker, normed, preferred_element_type=jnp.float32)
        .astype(jnp.bfloat16)
        .reshape(E, CAP, feat_local)
    )
    received = lax.all_gather(
        lax.all_to_all(outgoing, "sp", split_axis=0, concat_axis=0, tiled=True),
        "tp",
        axis=2,
        tiled=True,
    )
    local_experts = gate_experts.shape[0]
    sources = received.shape[0] // local_experts
    count = received.shape[1]
    rows = received.reshape(sources, local_experts, count, received.shape[2])
    gate_pre = jnp.minimum(
        jnp.einsum("sjcd,jdf->sjcf", rows, gate_experts, preferred_element_type=jnp.float32),
        clamp_limit,
    )
    up_pre = jnp.clip(
        jnp.einsum("sjcd,jdf->sjcf", rows, up_experts, preferred_element_type=jnp.float32),
        -clamp_limit,
        clamp_limit,
    )
    hidden = (gate_pre * jax.nn.sigmoid(swish_slope * gate_pre) * (up_pre + 1.0)).astype(
        jnp.bfloat16
    )
    partial_value = jnp.einsum(
        "sjcf,jfd->sjcd", hidden, down_experts, preferred_element_type=jnp.float32
    )
    summed = lax.psum_scatter(
        partial_value.astype(jnp.bfloat16), "tp", scatter_dimension=3, tiled=True
    )
    returned = lax.all_to_all(
        summed.reshape(sources * local_experts, count, summed.shape[3]),
        "sp",
        split_axis=0,
        concat_axis=0,
        tiled=True,
    )
    flat_back = returned.reshape(E * CAP, feat_local)
    picked = flat_back[slot_of].astype(jnp.float32).reshape(tok_rows, TOPK, feat_local)
    routed_sum = jnp.sum(picked * route_weights[:, :, None], axis=1)
    return (middle32 + routed_sum).astype(jnp.bfloat16)


MESH = pl.DeviceIdType.MESH
F32 = jnp.float32
BF16 = jnp.bfloat16


class Links:
    def __init__(self, send_sem, recv_sem):
        self.send_sem, self.recv_sem = send_sem, recv_sem
        self.numbers, self.started = {}, []

    def number(self, name):
        return self.numbers.setdefault(name, len(self.numbers))

    def send(self, src, dst, device, name):
        at = self.number(name)
        copy = pltpu.make_async_remote_copy(
            src_ref=src,
            dst_ref=dst,
            send_sem=self.send_sem.at[at],
            recv_sem=self.recv_sem.at[at],
            device_id=device,
            device_id_type=MESH,
        )
        copy.start()
        self.started.append(copy)

    def wait(self, dst, device, name):
        at = self.number(name)
        pltpu.make_async_remote_copy(
            src_ref=dst,
            dst_ref=dst,
            send_sem=self.send_sem.at[at],
            recv_sem=self.recv_sem.at[at],
            device_id=device,
            device_id_type=MESH,
        ).wait_recv()

    def finish(self):
        for copy in self.started:
            copy.wait_send()


def greet(devices):
    barrier = pltpu.get_barrier_semaphore()
    for device in devices:
        pl.semaphore_signal(barrier, inc=1, device_id=device, device_id_type=MESH)
    pl.semaphore_wait(barrier, len(devices))


def matches(slots, row, base, count):
    lane = lax.broadcasted_iota(jnp.int32, (count, slots.shape[1]), 0) + base
    return slots[row : row + 1, :] == lane.astype(F32)


def column(rows):
    ones = jnp.full((8, 128), 0.125, F32)
    wide = lax.dot_general(
        rows, ones, (((0,), (0,)), ((), ())), precision=lax.Precision.HIGHEST, preferred_element_type=F32
    )
    return wide[:, :1]


def row_totals(block):
    ones = jnp.ones((8, block.shape[1]), F32)
    return lax.dot_general(
        ones, block, (((1,), (1,)), ((), ())), precision=lax.Precision.HIGHEST, preferred_element_type=F32
    )


def front_kernel(
    n_sp,
    n_tp,
    conv_ref,
    chan_gain_ref,
    point_ref,
    mix_gain_ref,
    out_ref,
    resid_ref,
    norm_gain_ref,
    meta_ref,
    rows_ref,
    all_meta_ref,
    middle_ref,
    metas,
    stat,
    stat_in,
    square,
    square_in,
    parts,
    parts_in,
    mixed,
    own,
    full,
    pick,
    send_sem,
    recv_sem,
):
    s, t = lax.axis_index("sp"), lax.axis_index("tp")
    n_z = n_sp // 2
    tok, feat = conv_ref.shape
    half = tok // 2
    chan_total = feat * n_tp
    local = rows_ref.shape[0]
    cap = rows_ref.shape[1] // n_sp
    links = Links(send_sem, recv_sem)
    xp = t + 1 - 2 * lax.rem(t, 2)
    yp = lax.rem(t + 2, 4)
    dg = lax.rem(xp + 2, 4)
    sib = s + 1 - 2 * lax.rem(s, 2)
    zs = [lax.rem(s + 2 * k, n_sp) for k in range(n_z)]
    at_x, at_y, at_sib = {"sp": s, "tp": xp}, {"sp": s, "tp": yp}, {"sp": sib, "tp": t}
    tps = [lax.rem(t + d, n_tp) for d in range(n_tp)]
    sps = [lax.rem(s + d, n_sp) for d in range(n_sp)]
    greet([{"sp": s, "tp": p} for p in tps[1:]] + [{"sp": p, "tp": t} for p in sps[1:]])

    for d in range(1, n_sp):
        links.send(meta_ref, metas.at[s], {"sp": sps[d], "tp": t}, ("meta", n_sp - d))

    conv = conv_ref[...]
    stat[0:8, :] = row_totals(conv)
    stat[8:16, :] = row_totals(conv * conv)
    for d in range(1, n_tp):
        links.send(stat, stat_in.at[n_tp - d - 1], {"sp": s, "tp": tps[d]}, ("stat", n_tp - d))

    for d in range(n_sp):
        if d == 0:
            metas[s] = meta_ref[...]
        else:
            links.wait(metas.at[sps[d]], {"sp": sps[d], "tp": t}, ("meta", d))
        slots = metas[sps[d]]
        all_meta_ref[sps[d]] = slots
        found = matches(slots, 0, s * local * cap, local * cap)
        for k in range(1, TOPK):
            found = found | matches(slots, k, s * local * cap, local * cap)
        pick[sps[d]] = jnp.where(found, 1.0, 0.0).astype(BF16)

    total = stat[...]
    for d in range(1, n_tp):
        links.wait(stat_in.at[d - 1], {"sp": s, "tp": tps[d]}, ("stat", d))
        total = total + stat_in[d - 1]
    mean = column(total[0:8]) / chan_total
    var = column(total[8:16]) / chan_total - mean * mean
    v = (conv_ref[...] - mean) * lax.rsqrt(var + epsilon) * chan_gain_ref[...]
    act = (v / (1.0 + jnp.exp(-v))).astype(BF16)
    share = tok // n_tp
    parts[...] = (
        jnp.dot(act, point_ref[...], preferred_element_type=F32).astype(BF16).reshape(parts.shape)
    )
    for d in (2, 1, 3):
        links.send(parts.at[tps[d]], parts_in.at[n_tp - d - 1], {"sp": s, "tp": tps[d]}, ("part", n_tp - d))
    point = parts[t].astype(F32)
    for d in range(1, n_tp):
        links.wait(parts_in.at[d - 1], {"sp": s, "tp": tps[d]}, ("part", d))
        point = point + parts_in[d - 1].astype(F32)
    scale = lax.rsqrt(jnp.mean(point * point, axis=1, keepdims=True) + epsilon)
    mixed[t] = (point * scale * mix_gain_ref[...]).astype(BF16)
    for d in (2, 1, 3):
        links.send(mixed.at[t], mixed.at[t], {"sp": s, "tp": tps[d]}, ("mixed", n_tp - d))

    for d in (0, 1, 3, 2):
        if d:
            links.wait(mixed.at[tps[d]], {"sp": s, "tp": tps[d]}, ("mixed", d))
        here = pl.ds(pl.multiple_of(tps[d] * share, share), share)
        branch = jnp.dot(mixed[tps[d]], out_ref[...], preferred_element_type=F32)
        middle_ref[here, :] = (resid_ref[here, :].astype(F32) + branch).astype(BF16)

    middle = middle_ref[...].astype(F32)
    square[...] = row_totals(middle * middle)
    for d in (2, 1, 3):
        links.send(square, square_in.at[n_tp - d - 1], {"sp": s, "tp": tps[d]}, ("square", n_tp - d))
    total = square[...]
    for d in range(1, n_tp):
        links.wait(square_in.at[d - 1], {"sp": s, "tp": tps[d]}, ("square", d))
        total = total + square_in[d - 1]
    middle = middle_ref[...].astype(F32)
    own[...] = (
        middle * lax.rsqrt(column(total) / (feat * n_tp) + epsilon) * norm_gain_ref[...]
    ).astype(BF16)

    def place(source, block, value):
        picked = jnp.dot(pick[source], value, preferred_element_type=F32).astype(BF16)
        to = pl.ds(pl.multiple_of(source * cap, cap), cap)
        columns = pl.ds(pl.multiple_of(block * feat, feat), feat)
        rows_ref[:, to, columns] = picked.reshape(local, cap, feat)

    upper, lower = pl.ds(0, half), pl.ds(half, half)

    def spread(k):
        src = own if k == 0 else full.at[zs[k], t]
        links.send(src, full.at[zs[k], t], at_x, ("x", k))
        links.send(src, full.at[zs[k], t], at_y, ("y", k))
        if k == 0:
            for j in range(1, n_z):
                links.send(own, full.at[s, t], {"sp": zs[j], "tp": t}, ("z", n_z - j))
        links.send(src, full.at[zs[k], t], at_sib, ("sib", k, 0))

    def forward(k):
        links.wait(full.at[zs[k], xp], at_x, ("x", k))
        links.send(full.at[zs[k], xp, lower], full.at[zs[k], xp, lower], at_y, ("low", k))
        links.send(full.at[zs[k], xp], full.at[zs[k], xp], at_sib, ("sib", k, 1))
        links.wait(full.at[zs[k], yp], at_y, ("y", k))
        links.send(full.at[zs[k], yp, upper], full.at[zs[k], yp, upper], at_x, ("up", k))
        links.send(full.at[zs[k], yp], full.at[zs[k], yp], at_sib, ("sib", k, 2))

    def corner(k):
        links.wait(full.at[zs[k], dg, upper], at_x, ("up", k))
        links.wait(full.at[zs[k], dg, lower], at_y, ("low", k))
        links.send(full.at[zs[k], dg], full.at[zs[k], dg], at_sib, ("sib", k, 3))

    spread(0)
    order = [0]
    for j in range(1, n_z):
        for k in (j, n_z - j):
            if k not in order:
                order.append(k)
    place(s, t, own[...])
    others = (t, xp, yp, dg)

    def from_sibling(k):
        source = lax.rem(sib + 2 * k, n_sp)
        for i in range(4):
            links.wait(full.at[source, others[i]], at_sib, ("sib", k, i))
            place(source, others[i], full[source, others[i]])

    for i in range(1, n_z):
        k = order[i]
        links.wait(full.at[zs[k], t], {"sp": zs[k], "tp": t}, ("z", k))
        spread(k)
        place(zs[k], t, full[zs[k], t])
        forward(order[i - 1])
        for b in (xp, yp):
            place(zs[order[i - 1]], b, full[zs[order[i - 1]], b])
        if i >= 2:
            corner(order[i - 2])
            place(zs[order[i - 2]], dg, full[zs[order[i - 2]], dg])
    forward(order[n_z - 1])
    if n_z >= 2:
        corner(order[n_z - 2])
    for b in (xp, yp):
        place(zs[order[n_z - 1]], b, full[zs[order[n_z - 1]], b])
    if n_z >= 2:
        place(zs[order[n_z - 2]], dg, full[zs[order[n_z - 2]], dg])
    for k in order[:-1]:
        from_sibling(k)
    corner(order[n_z - 1])
    place(zs[order[n_z - 1]], dg, full[zs[order[n_z - 1]], dg])
    from_sibling(order[n_z - 1])
    links.finish()


def experts_kernel(rows_ref, gate_ref, up_ref, down_ref, y_ref, total):
    f = pl.program_id(1)
    rows = rows_ref[0]
    gate = jnp.minimum(jnp.dot(rows, gate_ref[0], preferred_element_type=F32), clamp_limit)
    up = jnp.clip(
        jnp.dot(rows, up_ref[0], preferred_element_type=F32), -clamp_limit, clamp_limit
    )
    hidden = (gate * jax.nn.sigmoid(swish_slope * gate) * (up + 1.0)).astype(BF16)
    part = jnp.dot(hidden, down_ref[0], preferred_element_type=F32)

    @pl.when(f == 0)
    def _():
        total[...] = part

    @pl.when(f > 0)
    def _():
        total[...] += part

    @pl.when(f == pl.num_programs(1) - 1)
    def _():
        y_ref[0] = total[...].astype(BF16)


def back_kernel(
    n_sp,
    n_tp,
    y_ref,
    all_meta_ref,
    middle_ref,
    result_ref,
    spread,
    mate_out,
    mate_in,
    acc,
    x_in,
    y_in,
    x_last,
    y_last,
    z_in,
    send_sem,
    recv_sem,
):
    s, t = lax.axis_index("sp"), lax.axis_index("tp")
    n_z = n_sp // 2
    tok, feat = middle_ref.shape
    half = tok // 2
    local = y_ref.shape[0]
    cap = y_ref.shape[1] // n_sp
    links = Links(send_sem, recv_sem)
    xp = t + 1 - 2 * lax.rem(t, 2)
    yp = lax.rem(t + 2, 4)
    dg = lax.rem(xp + 2, 4)
    sib = s + 1 - 2 * lax.rem(s, 2)
    zs = [lax.rem(s + 2 * k, n_sp) for k in range(n_z)]
    at_x, at_y, at_sib = {"sp": s, "tp": xp}, {"sp": s, "tp": yp}, {"sp": sib, "tp": t}
    greet([at_x, at_y, at_sib] + [{"sp": p, "tp": t} for p in zs[1:]])
    upper, lower = pl.ds(0, half), pl.ds(half, half)
    others = (dg, xp, yp, t)
    order = [k for k in range(1, n_z)] + [0]

    def weights_of(source):
        meta = all_meta_ref[source]
        weight = jnp.zeros((local * cap, tok), F32)
        for k in range(TOPK):
            here = matches(meta, k, s * local * cap, local * cap)
            weight = jnp.where(here, meta[TOPK + k : TOPK + k + 1, :], weight)
        spread[source] = weight.astype(BF16)

    def combined(source, block):
        to = pl.ds(pl.multiple_of(source * cap, cap), cap)
        columns = pl.ds(pl.multiple_of(block * feat, feat), feat)
        rows = y_ref[:, to, columns].reshape(local * cap, feat)
        return lax.dot_general(
            spread[source], rows, (((0,), (0,)), ((), ())), preferred_element_type=F32
        )

    for k in order:
        source = lax.rem(sib + 2 * k, n_sp)
        weights_of(source)
        for i in range(4):
            mate_out[k, i] = combined(source, others[i]).astype(BF16)
            links.send(mate_out.at[k, i], mate_in.at[k, i], at_sib, ("mate", k, i))
    for k in order:
        weights_of(zs[k])
        for i in range(4):
            value = combined(zs[k], others[i])
            links.wait(mate_in.at[k, i], at_sib, ("mate", k, i))
            acc[k, i] = (value + mate_in[k, i].astype(F32)).astype(BF16)
            if i == 0:
                links.send(acc.at[k, 0, upper], x_in.at[k, 1], at_x, ("x", k, 1))
                links.send(acc.at[k, 0, lower], y_in.at[k, 1], at_y, ("y", k, 1))
            if i == 1:
                links.send(acc.at[k, 1, upper], x_in.at[k, 0], at_x, ("x", k, 0))
            if i == 2:
                links.send(acc.at[k, 2, lower], y_in.at[k, 0], at_y, ("y", k, 0))

    def second(k):
        links.wait(x_in.at[k, 1], at_x, ("x", k, 1))
        acc[k, 2, upper] = (acc[k, 2, upper].astype(F32) + x_in[k, 1].astype(F32)).astype(BF16)
        links.send(acc.at[k, 2, upper], y_last.at[k], at_y, ("ylast", k))
        links.wait(y_in.at[k, 1], at_y, ("y", k, 1))
        acc[k, 1, lower] = (acc[k, 1, lower].astype(F32) + y_in[k, 1].astype(F32)).astype(BF16)
        links.send(acc.at[k, 1, lower], x_last.at[k], at_x, ("xlast", k))

    def third(k):
        links.wait(x_in.at[k, 0], at_x, ("x", k, 0))
        links.wait(y_in.at[k, 0], at_y, ("y", k, 0))
        links.wait(y_last.at[k], at_y, ("ylast", k))
        links.wait(x_last.at[k], at_x, ("xlast", k))
        up = acc[k, 3, upper].astype(F32) + x_in[k, 0].astype(F32) + y_last[k].astype(F32)
        low = acc[k, 3, lower].astype(F32) + y_in[k, 0].astype(F32) + x_last[k].astype(F32)
        return up, low

    for at in range(n_z + 1):
        if at < n_z:
            second(order[at])
        if at >= 1:
            k = order[at - 1]
            up, low = third(k)
            if k:
                acc[k, 3, upper] = up.astype(BF16)
                acc[k, 3, lower] = low.astype(BF16)
                links.send(acc.at[k, 3], z_in.at[n_z - k - 1], {"sp": zs[k], "tp": t}, ("z", n_z - k))
    for k in range(1, n_z):
        links.wait(z_in.at[k - 1], {"sp": zs[k], "tp": t}, ("z", k))
        up = up + z_in[k - 1, upper].astype(F32)
        low = low + z_in[k - 1, lower].astype(F32)
    result_ref[upper, :] = (middle_ref[upper, :].astype(F32) + up).astype(BF16)
    result_ref[lower, :] = (middle_ref[lower, :].astype(F32) + low).astype(BF16)
    links.finish()


def shards(
    resid,
    conv_value,
    conv_gate,
    depth_kernel,
    chan_gain,
    point_weight,
    mix_gain,
    out_weight,
    norm_gain,
    route_ids,
    route_weights,
    gate_experts,
    up_experts,
    down_experts,
):
    n_sp, n_tp = lax.axis_size("sp"), lax.axis_size("tp")
    n_z = n_sp // 2
    tok_rows, chan_local = conv_value.shape
    lookback = depth_kernel.shape[0] - 1
    gated = (conv_value.astype(F32) * jax.nn.sigmoid(conv_gate.astype(F32))).astype(BF16)
    earlier = from_behind(gated[tok_rows - lookback :], "sp", 1)
    padded = jnp.concatenate([earlier, gated], axis=0)
    conv = jnp.zeros((tok_rows, chan_local), F32)
    for tap in range(lookback + 1):
        conv = conv + padded[tap : tap + tok_rows].astype(F32) * depth_kernel[tap]

    flat_ids = route_ids.reshape(-1)
    expert_table = (flat_ids[:, None] == jnp.arange(E, dtype=jnp.int32)[None, :]).astype(jnp.int32)
    earlier_count = jnp.cumsum(expert_table, axis=0) - expert_table
    position = jnp.sum(earlier_count * expert_table, axis=1)
    slot_grid = (flat_ids * CAP + position).reshape(tok_rows, TOPK)
    meta = jnp.concatenate([slot_grid.T.astype(F32), route_weights.T], axis=0)

    local = gate_experts.shape[0]
    feat = resid.shape[1]
    share = tok_rows // n_tp
    half = tok_rows // 2
    vmem = pl.BlockSpec(memory_space=pltpu.VMEM)
    copies = 2 * (n_sp + 4 * n_tp + 12 * n_z)
    rows, metas, middle = pl.pallas_call(
        functools.partial(front_kernel, n_sp, n_tp),
        out_shape=(
            jax.ShapeDtypeStruct((local, n_sp * CAP, feat * n_tp), BF16),
            jax.ShapeDtypeStruct((n_sp,) + meta.shape, F32),
            jax.ShapeDtypeStruct((tok_rows, feat), BF16),
        ),
        in_specs=[vmem] * 8,
        out_specs=(vmem,) * 3,
        scratch_shapes=[
            pltpu.VMEM((n_sp,) + meta.shape, F32),
            pltpu.VMEM((16, tok_rows), F32),
            pltpu.VMEM((n_tp - 1, 16, tok_rows), F32),
            pltpu.VMEM((8, tok_rows), F32),
            pltpu.VMEM((n_tp - 1, 8, tok_rows), F32),
            pltpu.VMEM((n_tp, share, feat * n_tp), BF16),
            pltpu.VMEM((n_tp - 1, share, feat * n_tp), BF16),
            pltpu.VMEM((n_tp, share, feat * n_tp), BF16),
            pltpu.VMEM((tok_rows, feat), BF16),
            pltpu.VMEM((n_sp, n_tp, tok_rows, feat), BF16),
            pltpu.VMEM((n_sp, local * CAP, tok_rows), BF16),
            pltpu.SemaphoreType.DMA((copies,)),
            pltpu.SemaphoreType.DMA((copies,)),
        ],
        compiler_params=pltpu.CompilerParams(
            collective_id=0, has_side_effects=True, vmem_limit_bytes=30 * 1024 * 1024
        ),
    )(
        conv,
        chan_gain[None, :],
        point_weight,
        mix_gain[None, :],
        out_weight,
        resid,
        norm_gain[None, :],
        meta,
    )
    taken, width = rows.shape[1:]
    hidden_local = gate_experts.shape[2]
    tile = min(512, hidden_local)
    partial_value = pl.pallas_call(
        experts_kernel,
        grid=(local, hidden_local // tile),
        out_shape=jax.ShapeDtypeStruct(rows.shape, BF16),
        in_specs=[
            pl.BlockSpec((1, taken, width), lambda j, f: (j, 0, 0)),
            pl.BlockSpec((1, width, tile), lambda j, f: (j, 0, f)),
            pl.BlockSpec((1, width, tile), lambda j, f: (j, 0, f)),
            pl.BlockSpec((1, tile, width), lambda j, f: (j, f, 0)),
        ],
        out_specs=pl.BlockSpec((1, taken, width), lambda j, f: (j, 0, 0)),
        scratch_shapes=[pltpu.VMEM((taken, width), F32)],
        compiler_params=pltpu.CompilerParams(
            dimension_semantics=("arbitrary", "arbitrary"), vmem_limit_bytes=48 * 1024 * 1024
        ),
    )(rows, gate_experts, up_experts, down_experts)
    return pl.pallas_call(
        functools.partial(back_kernel, n_sp, n_tp),
        out_shape=jax.ShapeDtypeStruct((tok_rows, feat), BF16),
        in_specs=[vmem] * 3,
        out_specs=vmem,
        scratch_shapes=[
            pltpu.VMEM((n_sp, local * CAP, tok_rows), BF16),
            pltpu.VMEM((n_z, n_tp, tok_rows, feat), BF16),
            pltpu.VMEM((n_z, n_tp, tok_rows, feat), BF16),
            pltpu.VMEM((n_z, n_tp, tok_rows, feat), BF16),
            pltpu.VMEM((n_z, 2, half, feat), BF16),
            pltpu.VMEM((n_z, 2, half, feat), BF16),
            pltpu.VMEM((n_z, half, feat), BF16),
            pltpu.VMEM((n_z, half, feat), BF16),
            pltpu.VMEM((max(n_z - 1, 1), tok_rows, feat), BF16),
            pltpu.SemaphoreType.DMA((copies,)),
            pltpu.SemaphoreType.DMA((copies,)),
        ],
        compiler_params=pltpu.CompilerParams(
            collective_id=1, has_side_effects=True, vmem_limit_bytes=30 * 1024 * 1024
        ),
    )(partial_value, metas, middle)


def solution(mesh):
    body = shards if mesh.shape["tp"] == 4 and mesh.shape["sp"] % 2 == 0 else plain_shards
    in_specs = (
        P("sp", "tp"),
        P("sp", "tp"),
        P("sp", "tp"),
        P(None, "tp"),
        P("tp"),
        P("tp", None),
        P(),
        P(None, "tp"),
        P("tp"),
        P("sp", None),
        P("sp", None),
        P("sp", None, "tp"),
        P("sp", None, "tp"),
        P("sp", "tp", None),
    )
    out_specs = P("sp", "tp")
    return jax.shard_map(body, mesh=mesh, in_specs=in_specs, out_specs=out_specs, check_vma=False)
```
